32 devices in a mesh: ep: 8 (over z, x), tp: 4 (over y, core).
Axes of the slice: x: 2, y: 2, z: 4, core: 2. Of those that a mesh axis runs over, the one named last changes fastest.
Arguments:
- query_rows: bfloat16 [1536, 1024], P('ep', 'tp'), may hold values from -8 to 8
- key_rows: bfloat16 [1536, 1024], P('ep', 'tp'), may hold values from -8 to 8
- value_rows: bfloat16 [1536, 1024], P('ep', 'tp'), may hold values from -6 to 6
- lambdas: float32 [8], P('tp'), may hold values from 0.3 to 0.8
- head_gain: float32 [128], replicated, may hold values from 0.1 to 1.9
- w_out: bfloat16 [1024, 2048], replicated, may hold values from -0.1875 to 0.1875
- moe_rows: bfloat16 [4096, 2048], P('ep'), may hold values from -6 to 6
- ffn_gain: float32 [2048], replicated, may hold values from 0.1 to 1.9
- routes: int32 [4096, 2], P('ep'), may hold values from 0 to 7, all different within a row; in each aligned block of 128 rows (0 to 127, 128 to 255, ...) at most 64 rows name the same one
- group_logits: float32 [4096, 4], P('ep'), may hold values from -8 to 8
- pick_logits: float32 [4096, 2], P('ep'), may hold values from -8 to 8
- w_gate: bfloat16 [8, 2048, 1024], P('ep', None, 'tp'), may hold values from -0.125 to 0.125
- w_up: bfloat16 [8, 2048, 1024], P('ep', None, 'tp'), may hold values from -0.125 to 0.125
- w_down: bfloat16 [8, 1024, 2048], P('ep', 'tp'), may hold values from -0.75 to 0.75
Outputs:
- mixer_out: bfloat16 [1536, 2048], P(('ep', 'tp'))
- moe_out: bfloat16 [4096, 2048], P(('ep', 'tp'))
The draws below stay inside these ranges and needn't reach their ends.
Inputs may be any that keep to these rules, and one draw needn't show every extreme that they name: `routes`: each row names 2 different experts. In each aligned block of 128 rows (the rows of one device) no expert is named by more than 64 rows; some expert is named by exactly 64 rows of a block.
All inputs are finite; a program needn't handle non-finite values.
Results may differ from the reference program's by a relative error of at most 0.015.
Values may be sent and summed in bfloat16 or wider, within the bound.
A program may use at most 128 MiB of HBM per device.

```python
import math
import jax
import jax.numpy as jnp
import numpy as np
from jax import lax

D = 2048
HEADS = 8
HEAD_QK = 64
HEAD_V = 128
FFE = 1024
GROUPS = 4
TOP = 2
TOKQ = 128
EXPERTS = 8
CAP = 64
TOKA = 1536
TOKB = 4096
N_EP = 8
N_TP = 4


def drawn_pair(key):
    base = jax.random.fold_in(key, 41)
    first, second = jax.random.split(base, 2)
    columns = HEADS * 2 * HEAD_QK
    queries = jnp.clip(jax.random.normal(first, (TOKA, columns), jnp.float32) * 1.3, -6.0, 6.0)
    keys = jnp.clip(jax.random.normal(second, (TOKA, columns), jnp.float32) * 1.3, -6.0, 6.0)
    return (queries, keys)


def draw_query_rows(key, part):
    return drawn_pair(key)[0].astype(jnp.bfloat16)


def draw_key_rows(key, part):
    return drawn_pair(key)[1].astype(jnp.bfloat16)


def steps_of(rng, extent, shards, least, largest):
    factor_of, own = 1.0, jax.random.fold_in(rng, 6)
    for axis_at, shards_of in shards:
        heights = jnp.exp(jax.random.uniform(jax.random.fold_in(own, axis_at), (shards_of,), jnp.float32, least / len(shards), largest / len(shards)))
        factor_of = factor_of * jnp.repeat(heights, extent[axis_at] // shards_of).reshape([-1 if axis == axis_at else 1 for axis in range(len(extent))])
    return factor_of


def routed_block(own_key, own, number, rows, count, top, reach, lean):
    order = jax.random.permutation(own_key, count)
    crowded, usual = shares(count, rows * top, reach, lean, True), shares(count, rows * top, reach, lean, False)
    places = jnp.arange(count)

    def named(sizes, offset_by):
        used = int((sizes > 0).sum())
        fixed = max(1, used // 4)
        moved = fixed + (places - fixed + offset_by * (used - fixed)) % max(1, count - fixed)
        return jnp.zeros((count,), jnp.int32).at[order[jnp.where(places < fixed, places, moved)]].set(jnp.asarray(sizes, jnp.int32))

    sizes = jnp.where(number % 4 == 0, named(crowded, number // 4), named(usual, number - number // 4 - 1))
    mixed = jax.random.permutation(jax.random.fold_in(own, 3), count)
    donor, taker = mixed[0:count // 2 * 2:2], mixed[1:count // 2 * 2:2]
    margin = jnp.minimum(sizes[donor] - 1, reach - sizes[taker]) // 2
    margin = jnp.where((donor == order[0]) | (taker == order[0]) | (sizes[taker] == 0), 0, jnp.maximum(margin, 0))
    moved = jax.random.randint(jax.random.fold_in(own, 4), (count // 2,), 0, 1 << 20) % (margin + 1)
    sizes = sizes.at[donor].add(-moved).at[taker].add(moved)
    members = jnp.searchsorted(jnp.cumsum(sizes), jnp.arange(rows * top), side="right").astype(jnp.int32)
    table = members.reshape(top, rows).T
    table = table[jax.random.permutation(jax.random.fold_in(own, 1), rows)]
    offset_by = jax.random.randint(jax.random.fold_in(own, 2), (rows, 1), 0, top)
    return jnp.take_along_axis(table, (jnp.arange(top)[None, :] + offset_by) % top, axis=1)


def shares(amount, total, bound, skew, full):
    weights = [(1 << 20) // math.isqrt(rank ** skew) + 1 for rank in range(1, amount + 1)]
    largest = bound if full else min(bound, max(-(-total // amount), total * weights[0] // sum(weights)))
    least = 1 if total - largest >= amount - 1 else 0
    given, rest = [largest] + [least] * (amount - 1), total - largest - least * (amount - 1)
    while rest > 0:
        movable = [i for i in range(1, amount) if given[i] < largest] or [i for i in range(1, amount) if given[i] < bound]
        pool, left = sum([weights[i] for i in movable]), rest
        for i in movable:
            addition = min(bound - given[i], max(1, left * weights[i] // pool), rest)
            given[i] = given[i] + addition
            rest = rest - addition
    return np.array(given)


def scatter_about(own_key, extent, width, most, cuts=(), kind=jnp.bfloat16):
    level = steps_of(own_key, extent, cuts, -0.22, 0.18) if cuts else 1.0
    drawn = jax.random.normal(own_key, extent, jnp.float32) * width * level
    return jnp.minimum(jnp.maximum(drawn, -most), most).astype(kind)


def setup_inputs(seed: int = 0) -> dict:
    key_list = jax.random.split(jax.random.key(seed), 15)
    query_rows = draw_query_rows(jax.random.fold_in(key_list[14], 71), 0)
    key_rows = draw_key_rows(jax.random.fold_in(key_list[14], 71), 0)
    value_rows = scatter_about(key_list[2], (TOKA, HEADS * HEAD_V), 1.0, 6.0, ((0, 8), (1, 4)))
    lambdas = jnp.clip(0.3 + 0.5 * jax.random.uniform(key_list[3], (HEADS,), jnp.float32) ** steps_of(key_list[3], (HEADS,), ((0, 4),), -0.2, 0.2), 0.3, 0.8)
    head_gain = jnp.clip(1.0 + 0.18 * jax.random.normal(key_list[4], (HEAD_V,), jnp.float32), 0.1, 1.9)
    w_out = scatter_about(key_list[5], (HEADS * HEAD_V, D), (HEADS * HEAD_V) ** -0.5, 0.1875)
    moe_rows = scatter_about(key_list[6], (TOKB, D), 1.0, 6.0, ((0, 8),))
    ffn_gain = jnp.clip(1.0 + 0.18 * jax.random.normal(key_list[7], (D,), jnp.float32), 0.1, 1.9)
    routes_keys = jax.random.split(jax.random.fold_in(key_list[8], 1), TOKB // TOKQ)
    routes_turns = jax.random.permutation(jax.random.fold_in(key_list[8], 3), TOKB // TOKQ)
    routes = jax.vmap(lambda own, number: routed_block(jax.random.fold_in(key_list[8], 2), own, number, TOKQ, EXPERTS, TOP, CAP, 1))(routes_keys, routes_turns).reshape((TOKB, TOP))
    group_logits = scatter_about(key_list[9], (TOKB, GROUPS), 2.0, 8.0, ((0, 8),), jnp.float32)
    pick_logits = scatter_about(key_list[10], (TOKB, TOP), 1.5, 8.0, ((0, 8),), jnp.float32)
    w_gate = scatter_about(key_list[11], (EXPERTS, D, FFE), D ** -0.5, 0.125, ((0, 8), (2, 4)))
    w_up = scatter_about(key_list[12], (EXPERTS, D, FFE), D ** -0.5, 0.125, ((0, 8), (2, 4)))
    w_down = scatter_about(key_list[13], (EXPERTS, FFE, D), (FFE // 16) ** -0.5, 0.75, ((0, 8), (1, 4)))
    return dict(query_rows=query_rows, key_rows=key_rows, value_rows=value_rows, lambdas=lambdas, head_gain=head_gain, w_out=w_out, moe_rows=moe_rows, ffn_gain=ffn_gain, routes=routes, group_logits=group_logits, pick_logits=pick_logits, w_gate=w_gate, w_up=w_up, w_down=w_down)


EPS = 1e-06
HEAD_SCALE = 0.8

def rms_rows(values, gain):
    squared = lax.optimization_barrier(jnp.mean(values * values, axis=-1, keepdims=True))
    return values * lax.rsqrt(squared + EPS) * gain

def attend(query_rows, key_rows, value_rows, lambdas, head_gain):
    token_count = query_rows.shape[0]
    block_rows = math.gcd(token_count, 128)
    keys = key_rows.astype(jnp.float32).reshape(token_count, HEADS, 2, HEAD_QK)
    values = value_rows.astype(jnp.float32).reshape(token_count, HEADS, HEAD_V)
    queries = query_rows.astype(jnp.float32).reshape(token_count // block_rows, block_rows, HEADS, 2, HEAD_QK)

    def one_block(query_block):
        scores = jnp.einsum('qhmd,khmd->hmqk', query_block, keys, precision=lax.Precision.HIGHEST) * HEAD_QK ** (-0.5)
        weights = jnp.exp(scores - lax.optimization_barrier(jnp.max(scores, axis=-1, keepdims=True)))
        totals = lax.optimization_barrier(jnp.sum(weights, axis=-1))
        rounded = lax.optimization_barrier(weights.astype(jnp.bfloat16)).astype(jnp.float32)
        sums = jnp.einsum('hmqk,khv->hmqv', rounded, values, precision=lax.Precision.HIGHEST)
        per_head = sums[:, 0] / totals[:, 0, :, None] - lambdas[:, None, None] * sums[:, 1] / totals[:, 1, :, None]
        normed = rms_rows(per_head, head_gain) * HEAD_SCALE
        return jnp.transpose(normed, (1, 0, 2)).reshape(block_rows, HEADS * HEAD_V).astype(jnp.bfloat16)
    return lax.map(one_block, queries).reshape(token_count, HEADS * HEAD_V)

def experts_part(moe_rows, ffn_gain, routes, group_logits, pick_logits, w_gate, w_up, w_down):
    model_width = moe_rows.shape[1]
    quarters = N_EP * N_TP
    normed = rms_rows(moe_rows.astype(jnp.float32), ffn_gain).astype(jnp.bfloat16)
    flattened = routes.reshape(quarters, TOKQ * TOP)
    onehot = (flattened[..., None] == jnp.arange(EXPERTS, dtype=jnp.int32)).astype(jnp.int32)
    before = jnp.cumsum(onehot, axis=1) - onehot
    ranking = lax.optimization_barrier(jnp.sum(before * onehot, axis=-1))
    slots = (flattened * quarters + jnp.arange(quarters, dtype=jnp.int32)[:, None]) * CAP + ranking
    source_rows = jnp.repeat(jnp.arange(TOKB, dtype=jnp.int32), TOP)
    buffer_rows = jnp.zeros((EXPERTS * quarters * CAP, model_width), jnp.bfloat16)
    buffer_rows = buffer_rows.at[slots.reshape(-1)].set(normed[source_rows])
    buffer_rows = buffer_rows.reshape(EXPERTS, quarters * CAP, model_width)
    unit_block = FFE // N_TP

    def run_expert(packed):
        expert_rows, gate_weight, up_weight, down_weight = packed
        gate_part = jnp.dot(expert_rows, gate_weight, preferred_element_type=jnp.float32)
        up_part = jnp.dot(expert_rows, up_weight, preferred_element_type=jnp.float32)
        hidden = (jax.nn.silu(gate_part) * up_part).astype(jnp.bfloat16)
        split_hidden = hidden.astype(jnp.float32).reshape(-1, N_TP, unit_block)
        split_down = down_weight.astype(jnp.float32).reshape(N_TP, unit_block, model_width)
        parts = jnp.einsum('rnf,nfd->nrd', split_hidden, split_down, precision=lax.Precision.HIGHEST)
        parts = lax.optimization_barrier(parts.astype(jnp.bfloat16)).astype(jnp.float32)
        return lax.optimization_barrier(jnp.sum(parts, axis=0)).astype(jnp.bfloat16)
    outputs = lax.map(run_expert, (buffer_rows, w_gate, w_up, w_down))
    picked = outputs.reshape(-1, model_width)[slots.reshape(-1)].reshape(TOKB, TOP, model_width)
    group_prob = jax.nn.softmax(group_logits, axis=-1)
    group_index = routes // (EXPERTS // GROUPS)
    matches = (group_index[..., None] == jnp.arange(GROUPS, dtype=jnp.int32)).astype(jnp.float32)
    group_share = lax.optimization_barrier(jnp.sum(group_prob[:, None, :] * matches, axis=-1))
    gate_values = group_share * jax.nn.softmax(pick_logits, axis=-1)
    return lax.optimization_barrier(jnp.sum(gate_values[..., None] * picked.astype(jnp.float32), axis=1)).astype(jnp.bfloat16)

def reference(query_rows, key_rows, value_rows, lambdas, head_gain, w_out, moe_rows, ffn_gain, routes, group_logits, pick_logits, w_gate, w_up, w_down):
    attended = attend(query_rows, key_rows, value_rows, lambdas, head_gain)
    mixer_out = jnp.dot(attended, w_out, preferred_element_type=jnp.float32).astype(jnp.bfloat16)
    moe_out = experts_part(moe_rows, ffn_gain, routes, group_logits, pick_logits, w_gate, w_up, w_down)
    return (mixer_out, moe_out)
```

```python
import functools

import jax
import jax.numpy as jnp
from jax import lax
from jax.experimental import pallas as pl
from jax.experimental.pallas import tpu as pltpu
from jax.sharding import PartitionSpec as P

EPS = 1e-06
HEAD_SCALE = 0.8
CHUNKS = 4
MESH = pl.DeviceIdType.MESH
F32 = jnp.float32
BF16 = jnp.bfloat16


def flat_rows(values):
    blocks, rows, columns = values.shape
    if rows % 16:
        return values.astype(F32).reshape(blocks * rows, columns).astype(values.dtype)
    return values.reshape(blocks * rows, columns)


def split_rows(values, rows):
    columns = values.shape[1]
    if rows % 16:
        return values.reshape(-1, rows, columns).astype(BF16)
    return values.astype(BF16).reshape(-1, rows, columns)


def kernel(
    n,
    tp,
    dims,
    query_ref,
    key_ref,
    value_ref,
    lambda_ref,
    head_gain_ref,
    w_out_ref,
    moe_ref,
    ffn_gain_ref,
    routes_ref,
    groups_ref,
    picks_ref,
    gate_ref,
    up_ref,
    down_ref,
    mixer_ref,
    out_ref,
    rows_buf,
    sent,
    arrived,
    w_gate,
    w_up,
    w_down,
    keys,
    values,
    w_out,
    attended,
    collected,
    hidden,
    results,
    returned,
    local_sem,
    weight_send,
    weight_recv,
    row_send,
    row_recv,
    kv_send,
    kv_recv,
    back_send,
    back_recv,
    head_send,
    head_recv,
):
    token_count, local_heads, head_qk, head_v, quarter, capacity, group_count = dims
    ep = lax.axis_index("ep")
    me = lax.axis_index("tp")
    mate = me + 1 - 2 * lax.rem(me, 2)
    across = lax.rem(me + tp // 2, tp)
    diagonal = lax.rem(mate + tp // 2, tp)
    beside = ep + 1 - 2 * lax.rem(ep, 2)
    half = n // 2
    width = out_ref.shape[1]
    part = width // CHUNKS

    def remote(source, target, send, recv, device):
        return pltpu.make_async_remote_copy(
            src_ref=source,
            dst_ref=target,
            send_sem=send,
            recv_sem=recv,
            device_id=device,
            device_id_type=MESH,
        )

    own_rows = pltpu.make_async_copy(
        moe_ref.at[pl.ds(pl.multiple_of(me * quarter, quarter), quarter)], rows_buf, local_sem.at[0]
    )
    own_rows.start()
    locals_ = [
        pltpu.make_async_copy(gate_ref.at[0], w_gate.at[0], local_sem.at[1]),
        pltpu.make_async_copy(up_ref.at[0], w_up.at[0], local_sem.at[2]),
        pltpu.make_async_copy(down_ref.at[0], w_down.at[0], local_sem.at[3]),
        pltpu.make_async_copy(key_ref, keys.at[0], local_sem.at[4]),
        pltpu.make_async_copy(value_ref, values.at[0], local_sem.at[5]),
        pltpu.make_async_copy(w_out_ref, w_out, local_sem.at[6]),
    ]
    for copy in locals_:
        copy.start()

    barrier = pltpu.get_barrier_semaphore()
    for peer in (mate, across, diagonal):
        pl.semaphore_signal(barrier, inc=1, device_id=(ep, peer), device_id_type=MESH)

    def greet(step, carry):
        pl.semaphore_signal(
            barrier, inc=1, device_id=(lax.rem(ep + step, n), me), device_id_type=MESH
        )
        return carry

    lax.fori_loop(1, n, greet, 0)
    pl.semaphore_wait(barrier, n - 1 + 3)

    def columns(number):
        return pl.ds(number * part, part)

    def weight_copies(place, first):
        device = (ep, across if place == 2 else mate)
        sources = (
            (gate_ref.at[0], up_ref.at[0], down_ref.at[0])
            if first
            else (w_gate.at[2], w_up.at[2], w_down.at[2])
        )
        base = place - 1
        copies = [
            remote(
                sources[0],
                w_gate.at[place],
                weight_send.at[base, 0],
                weight_recv.at[base, 0],
                device,
            ),
            remote(
                sources[1],
                w_up.at[place],
                weight_send.at[base, 1],
                weight_recv.at[base, 1],
                device,
            ),
        ]
        for number in range(CHUNKS):
            copies.append(
                remote(
                    sources[2].at[:, columns(number)],
                    w_down.at[place, :, columns(number)],
                    weight_send.at[base, 2 + number],
                    weight_recv.at[base, 2 + number],
                    device,
                )
            )
        return copies

    to_across = weight_copies(2, True)
    to_mate = weight_copies(1, True)
    relayed = weight_copies(3, False)
    for copy in to_across:
        copy.start()
    for copy in to_mate:
        copy.start()

    own = pl.ds(pl.multiple_of(me * quarter, quarter), quarter)
    routes = routes_ref[own, :]
    first, second = routes[:, 0:1], routes[:, 1:2]
    lanes = lax.broadcasted_iota(jnp.int32, (quarter, 128), 1)
    away = [lax.rem(pick - ep + n, n) for pick in (first, second)]
    named = jnp.where((lanes == away[0]) | (lanes == away[1]), 1.0, 0.0)
    row_at = lax.broadcasted_iota(jnp.int32, (quarter, quarter), 0)
    column_at = lax.broadcasted_iota(jnp.int32, (quarter, quarter), 1)
    earlier = jnp.where(column_at < row_at, 1.0, 0.0).astype(BF16)
    before = jnp.dot(earlier, named.astype(BF16), preferred_element_type=F32)
    places = [
        away_k * capacity
        + jnp.sum(jnp.where(lanes == away_k, before, 0.0), axis=1, keepdims=True).astype(jnp.int32)
        for away_k in away
    ]
    slot_at = lax.broadcasted_iota(jnp.int32, (quarter, n * capacity), 1)
    pick_of = [jnp.where(slot_at == place, 1.0, 0.0) for place in places]
    spread = (pick_of[0] + pick_of[1]).astype(BF16)

    own_rows.wait()
    tokens = rows_buf[...].astype(F32)
    squared = jnp.mean(tokens * tokens, axis=-1, keepdims=True)
    normed = (tokens * lax.rsqrt(squared + EPS) * ffn_gain_ref[...]).astype(BF16)
    slotted = lax.dot_general(
        spread, normed, (((0,), (0,)), ((), ())), preferred_element_type=F32
    )
    sent[...] = split_rows(slotted, capacity)

    def row_copy(step):
        return remote(
            sent.at[step],
            arrived.at[step],
            row_send.at[step],
            row_recv.at[step],
            (lax.rem(ep + step, n), me),
        )

    def start_rows(step, carry):
        row_copy(step).start()
        return carry

    lax.fori_loop(1, n, start_rows, 0)
    arrived[0] = sent[0]

    def kv_copies(step, relay):
        to = step + half if relay else step
        device = (beside, me) if relay else (lax.rem(ep + 2 * step, n), me)
        key_source = keys.at[step] if relay else key_ref
        value_source = values.at[step] if relay else value_ref
        return (
            remote(key_source, keys.at[to], kv_send.at[0, to], kv_recv.at[0, to], device),
            remote(value_source, values.at[to], kv_send.at[1, to], kv_recv.at[1, to], device),
        )

    def start_kv(step, carry):
        for copy in kv_copies(step, False):
            copy.start()
        return carry

    lax.fori_loop(1, half, start_kv, 0)

    groups = groups_ref[own, :]
    group_weights = jnp.exp(groups - jnp.max(groups, axis=-1, keepdims=True))
    group_prob = group_weights / jnp.sum(group_weights, axis=-1, keepdims=True)
    picks = picks_ref[own, :]
    pick_weights = jnp.exp(picks - jnp.max(picks, axis=-1, keepdims=True))
    pick_prob = pick_weights / jnp.sum(pick_weights, axis=-1, keepdims=True)
    group_at = lax.broadcasted_iota(jnp.int32, groups.shape, 1)
    gates = [
        jnp.sum(jnp.where(group_at == pick // (n // group_count), group_prob, 0.0), axis=1, keepdims=True)
        * pick_prob[:, k : k + 1]
        for k, pick in enumerate((first, second))
    ]

    for copy in locals_:
        copy.wait()

    to_across[0].wait_recv()
    relayed[0].start()

    def wait_rows(step, carry):
        row_copy(step).wait_recv()
        return carry

    lax.fori_loop(1, n, wait_rows, 0)
    units = gate_ref.shape[2]

    def hide(place):
        rows = flat_rows(arrived[...])
        gate_part = jnp.dot(rows, w_gate[place], preferred_element_type=F32)
        up_part = jnp.dot(rows, w_up[place], preferred_element_type=F32)
        hidden[place] = (gate_part / (1.0 + jnp.exp(-gate_part)) * up_part).astype(BF16)

    hide(0)
    to_mate[0].wait_recv()
    to_mate[1].wait_recv()
    hide(1)
    to_across[1].wait_recv()
    relayed[1].start()
    hide(2)
    relayed[0].wait_recv()
    relayed[1].wait_recv()
    hide(3)

    def back_copy(number, step):
        return remote(
            results.at[number, step],
            returned.at[number, step],
            back_send.at[number, step],
            back_recv.at[number, step],
            (lax.rem(ep - step + n, n), me),
        )

    for number in range(CHUNKS):
        to_across[2 + number].wait_recv()
        relayed[2 + number].start()
        to_mate[2 + number].wait_recv()
        total = jnp.zeros((n * capacity, part), F32)
        for place in range(3):
            total += jnp.dot(
                hidden[place], w_down[place, :, columns(number)], preferred_element_type=F32
            )
        relayed[2 + number].wait_recv()
        total += jnp.dot(hidden[3], w_down[3, :, columns(number)], preferred_element_type=F32)
        results[number] = split_rows(total, capacity)

        def start_back(step, carry):
            back_copy(number, step).start()
            return carry

        lax.fori_loop(1, n, start_back, 0)
        returned[number, 0] = results[number, 0]

    def relay_kv(step, carry):
        for copy in kv_copies(step, False):
            copy.wait_recv()
        for copy in kv_copies(step, True):
            copy.start()
        return carry

    for copy in kv_copies(0, True):
        copy.start()
    lax.fori_loop(1, half, relay_kv, 0)

    def wait_kv(step, carry):
        for copy in kv_copies(step, True):
            copy.wait_recv()
        return carry

    lax.fori_loop(0, half, wait_kv, 0)

    blocks = min(n, 8)
    scale = head_qk**-0.5
    share = token_count // tp
    for head in range(local_heads):
        averaged = []
        for way in range(2):
            at = (2 * head + way) * head_qk
            query = query_ref[:, at : at + head_qk]

            def scored(step):
                key_rows = keys[pl.ds(step * blocks, blocks), :, at : at + head_qk]
                return (
                    lax.dot_general(
                        query,
                        key_rows.reshape(blocks * token_count, head_qk),
                        (((1,), (1,)), ((), ())),
                        preferred_element_type=F32,
                    )
                    * scale
                )

            def absorb(step, carry):
                top, mass, sums = carry
                scores = scored(step)
                new_top = jnp.maximum(top, jnp.max(scores, axis=-1, keepdims=True))
                factor = jnp.exp(top - new_top)
                weights = jnp.exp(scores - new_top)
                value_rows = values[
                    pl.ds(step * blocks, blocks), :, head * head_v : (head + 1) * head_v
                ].reshape(blocks * token_count, head_v)
                mass = mass * factor + jnp.sum(weights, axis=-1, keepdims=True)
                sums = sums * factor + jnp.dot(
                    weights.astype(BF16), value_rows, preferred_element_type=F32
                )
                return new_top, mass, sums

            start = (
                jnp.full((token_count, 1), -1e30, F32),
                jnp.zeros((token_count, 1), F32),
                jnp.zeros((token_count, head_v), F32),
            )
            if n == blocks:
                top, mass, sums = absorb(0, start)
            else:
                top, mass, sums = lax.fori_loop(0, n // blocks, absorb, start)
            averaged.append(sums / mass)
        lambda_at = lambda_ref[0, head]
        per_head = averaged[0] - lambda_at * averaged[1]
        squares = jnp.mean(per_head * per_head, axis=-1, keepdims=True)
        normed_head = per_head * lax.rsqrt(squares + EPS) * head_gain_ref[...] * HEAD_SCALE
        attended[:, :, head * head_v : (head + 1) * head_v] = normed_head.astype(BF16).reshape(
            tp, share, head_v
        )

    head_copies = []
    for step in range(1, tp):
        head_copies.append(
            remote(
                attended.at[lax.rem(me + step, tp)],
                collected.at[step],
                head_send.at[step],
                head_recv.at[step],
                (ep, lax.rem(me + step, tp)),
            )
        )
    for copy in head_copies:
        copy.start()
    collected[0] = attended[me]
    depth = local_heads * head_v
    for copy in head_copies:
        copy.wait_recv()
    mixed = jnp.zeros((share, width), F32)
    for step in range(tp):
        from_tp = lax.rem(me - step + tp, tp)
        mixed += jnp.dot(
            collected[step],
            w_out[pl.ds(pl.multiple_of(from_tp * depth, depth), depth), :],
            preferred_element_type=F32,
        )
    mixer_ref[...] = mixed.astype(BF16)

    choose = [pick.astype(BF16) for pick in pick_of]
    for number in range(CHUNKS):

        def wait_back(step, carry):
            back_copy(number, step).wait_recv()
            return carry

        lax.fori_loop(1, n, wait_back, 0)
        rows = flat_rows(returned[number])
        combined = gates[0] * jnp.dot(choose[0], rows, preferred_element_type=F32)
        combined += gates[1] * jnp.dot(choose[1], rows, preferred_element_type=F32)
        out_ref[:, number * part : (number + 1) * part] = combined.astype(BF16)

    for copy in to_across + to_mate + relayed + head_copies:
        copy.wait_send()

    def drain(step, carry):
        row_copy(step).wait_send()
        for number in range(CHUNKS):
            back_copy(number, step).wait_send()
        return carry

    lax.fori_loop(1, n, drain, 0)

    def drain_kv(step, carry):
        for copy in kv_copies(step, True):
            copy.wait_send()
        return carry

    lax.fori_loop(0, half, drain_kv, 0)

    def drain_outer(step, carry):
        for copy in kv_copies(step, False):
            copy.wait_send()
        return carry

    lax.fori_loop(1, half, drain_outer, 0)


def local(
    n,
    tp,
    query_rows,
    key_rows,
    value_rows,
    lambdas,
    head_gain,
    w_out,
    moe_rows,
    ffn_gain,
    routes,
    group_logits,
    pick_logits,
    w_gate,
    w_up,
    w_down,
):
    token_count = query_rows.shape[0]
    local_heads = lambdas.shape[1]
    head_qk = query_rows.shape[1] // (2 * local_heads)
    head_v = value_rows.shape[1] // local_heads
    width = moe_rows.shape[1]
    quarter = moe_rows.shape[0] // tp
    capacity = max(2, 2 * routes.shape[1] * quarter // n)
    units = w_gate.shape[2]
    part = width // CHUNKS
    share = token_count // tp
    dims = (token_count, local_heads, head_qk, head_v, quarter, capacity, group_logits.shape[1])
    vmem = pl.BlockSpec(memory_space=pltpu.VMEM)
    anywhere = pl.BlockSpec(memory_space=pl.ANY)
    dma = pltpu.SemaphoreType.DMA
    return pl.pallas_call(
        functools.partial(kernel, n, tp, dims),
        out_shape=(
            jax.ShapeDtypeStruct((share, width), BF16),
            jax.ShapeDtypeStruct((quarter, width), BF16),
        ),
        in_specs=[
            vmem,
            anywhere,
            anywhere,
            pl.BlockSpec(memory_space=pltpu.SMEM),
            vmem,
            anywhere,
            anywhere,
            vmem,
            vmem,
            vmem,
            vmem,
            anywhere,
            anywhere,
            anywhere,
        ],
        out_specs=(vmem, vmem),
        scratch_shapes=[
            pltpu.VMEM((quarter, width), BF16),
            pltpu.VMEM((n, capacity, width), BF16),
            pltpu.VMEM((n, capacity, width), BF16),
            pltpu.VMEM((4, width, units), BF16),
            pltpu.VMEM((4, width, units), BF16),
            pltpu.VMEM((4, units, width), BF16),
            pltpu.VMEM((n, token_count, key_rows.shape[1]), BF16),
            pltpu.VMEM((n, token_count, value_rows.shape[1]), BF16),
            pltpu.VMEM(w_out.shape, BF16),
            pltpu.VMEM((tp, share, local_heads * head_v), BF16),
            pltpu.VMEM((tp, share, local_heads * head_v), BF16),
            pltpu.VMEM((4, n * capacity, units), BF16),
            pltpu.VMEM((CHUNKS, n, capacity, part), BF16),
            pltpu.VMEM((CHUNKS, n, capacity, part), BF16),
            dma((7,)),
            dma((3, 2 + CHUNKS)),
            dma((3, 2 + CHUNKS)),
            dma((n,)),
            dma((n,)),
            dma((2, n)),
            dma((2, n)),
            dma((CHUNKS, n)),
            dma((CHUNKS, n)),
            dma((tp,)),
            dma((tp,)),
        ],
        compiler_params=pltpu.CompilerParams(
            collective_id=0, has_side_effects=True, vmem_limit_bytes=60 * 1024 * 1024
        ),
    )(
        query_rows,
        key_rows,
        value_rows,
        lambdas,
        head_gain.reshape(1, -1),
        w_out,
        moe_rows,
        ffn_gain.reshape(1, -1),
        routes,
        group_logits,
        pick_logits,
        w_gate,
        w_up,
        w_down,
    )


def solution(mesh):
    inner = jax.shard_map(
        functools.partial(local, mesh.shape["ep"], mesh.shape["tp"]),
        mesh=mesh,
        in_specs=(
            P("ep", "tp"),
            P("ep", "tp"),
            P("ep", "tp"),
            P(None, "tp"),
            P(),
            P(),
            P("ep", None),
            P(),
            P("ep", None),
            P("ep", None),
            P("ep", None),
            P("ep", None, "tp"),
            P("ep", None, "tp"),
            P("ep", "tp", None),
        ),
        out_specs=(P(("ep", "tp"), None), P(("ep", "tp"), None)),
        check_vma=False,
    )

    def whole(query_rows, key_rows, value_rows, lambdas, *rest):
        return inner(query_rows, key_rows, value_rows, lambdas.reshape(1, -1), *rest)

    return whole
```

```python
import functools

import jax
import jax.numpy as jnp
from jax import lax
from jax.experimental import pallas as pl
from jax.experimental.pallas import tpu as pltpu
from jax.sharding import PartitionSpec as P

EPS = 1e-06
HEAD_SCALE = 0.8
CHUNKS = 4
MESH = pl.DeviceIdType.MESH
F32 = jnp.float32
BF16 = jnp.bfloat16


def flat_rows(values):
    blocks, rows, columns = values.shape
    if rows % 16:
        return values.astype(F32).reshape(blocks * rows, columns).astype(values.dtype)
    return values.reshape(blocks * rows, columns)


def split_rows(values, rows):
    columns = values.shape[1]
    if rows % 16:
        return values.reshape(-1, rows, columns).astype(BF16)
    return values.astype(BF16).reshape(-1, rows, columns)


def kernel(
    n,
    tp,
    dims,
    query_ref,
    key_ref,
    value_ref,
    lambda_ref,
    head_gain_ref,
    w_out_ref,
    moe_ref,
    ffn_gain_ref,
    routes_ref,
    groups_ref,
    picks_ref,
    gate_ref,
    up_ref,
    down_ref,
    mixer_ref,
    out_ref,
    rows_buf,
    marks,
    line,
    sent,
    arrived,
    w_gate,
    w_up,
    w_down,
    keys,
    values,
    w_out,
    attended,
    collected,
    hidden,
    results,
    returned,
    local_sem,
    line_send,
    line_recv,
    weight_send,
    weight_recv,
    row_send,
    row_recv,
    kv_send,
    kv_recv,
    back_send,
    back_recv,
    head_send,
    head_recv,
):
    token_count, local_heads, head_qk, head_v, quarter, capacity, group_count = dims
    ep = lax.axis_index("ep")
    me = lax.axis_index("tp")
    mate = me + 1 - 2 * lax.rem(me, 2)
    across = lax.rem(me + tp // 2, tp)
    diagonal = lax.rem(mate + tp // 2, tp)
    beside = ep + 1 - 2 * lax.rem(ep, 2)
    half = n // 2
    at, side = ep // 2, lax.rem(ep, 2)
    width = out_ref.shape[1]
    part = width // CHUNKS

    def remote(source, target, send, recv, device):
        return pltpu.make_async_remote_copy(
            src_ref=source,
            dst_ref=target,
            send_sem=send,
            recv_sem=recv,
            device_id=device,
            device_id_type=MESH,
        )

    own_rows = pltpu.make_async_copy(
        moe_ref.at[pl.ds(pl.multiple_of(me * quarter, quarter), quarter)], rows_buf, local_sem.at[0]
    )
    own_rows.start()
    locals_ = [
        pltpu.make_async_copy(gate_ref.at[0], w_gate.at[0], local_sem.at[1]),
        pltpu.make_async_copy(up_ref.at[0], w_up.at[0], local_sem.at[2]),
        pltpu.make_async_copy(down_ref.at[0], w_down.at[0], local_sem.at[3]),
        pltpu.make_async_copy(key_ref, keys.at[ep], local_sem.at[4]),
        pltpu.make_async_copy(value_ref, values.at[ep], local_sem.at[5]),
        pltpu.make_async_copy(w_out_ref, w_out, local_sem.at[6]),
    ]
    for copy in locals_:
        copy.start()

    barrier = pltpu.get_barrier_semaphore()
    for peer in (mate, across, diagonal):
        pl.semaphore_signal(barrier, inc=1, device_id=(ep, peer), device_id_type=MESH)

    def greet(step, carry):
        pl.semaphore_signal(
            barrier, inc=1, device_id=(lax.rem(ep + step, n), me), device_id_type=MESH
        )
        return carry

    lax.fori_loop(1, n, greet, 0)
    pl.semaphore_wait(barrier, n - 1 + 3)

    def columns(number):
        return pl.ds(number * part, part)

    def weight_copies(place, first):
        device = (ep, across if place == 2 else mate)
        sources = (
            (gate_ref.at[0], up_ref.at[0], down_ref.at[0])
            if first
            else (w_gate.at[2], w_up.at[2], w_down.at[2])
        )
        base = place - 1
        copies = [
            remote(
                sources[0],
                w_gate.at[place],
                weight_send.at[base, 0],
                weight_recv.at[base, 0],
                device,
            ),
            remote(
                sources[1],
                w_up.at[place],
                weight_send.at[base, 1],
                weight_recv.at[base, 1],
                device,
            ),
        ]
        for number in range(CHUNKS):
            copies.append(
                remote(
                    sources[2].at[:, columns(number)],
                    w_down.at[place, :, columns(number)],
                    weight_send.at[base, 2 + number],
                    weight_recv.at[base, 2 + number],
                    device,
                )
            )
        return copies

    to_across = weight_copies(2, True)
    to_mate = weight_copies(1, True)
    relayed = weight_copies(3, False)
    for copy in to_across:
        copy.start()
    for copy in to_mate:
        copy.start()

    own = pl.ds(pl.multiple_of(me * quarter, quarter), quarter)
    routes = routes_ref[:, own]
    first, second = routes[0:1, :], routes[1:2, :]
    experts = lax.broadcasted_iota(jnp.int32, (n, quarter), 0)
    named = jnp.where((experts == first) | (experts == second), 1.0, 0.0)
    row_at = lax.broadcasted_iota(jnp.int32, (quarter, quarter), 0)
    column_at = lax.broadcasted_iota(jnp.int32, (quarter, quarter), 1)
    earlier = jnp.where(row_at < column_at, 1.0, 0.0).astype(BF16)
    before = jnp.dot(named.astype(BF16), earlier, preferred_element_type=F32)
    slots = [
        (pick * capacity).astype(F32)
        + jnp.sum(jnp.where(experts == pick, before, 0.0), axis=0, keepdims=True)
        for pick in (first, second)
    ]
    mark_at = lax.broadcasted_iota(jnp.int32, (8, quarter), 0)
    marks[at] = jnp.where(mark_at == 0, slots[0], slots[1])

    own_rows.wait()
    tokens = rows_buf[...].astype(F32)
    squared = jnp.mean(tokens * tokens, axis=-1, keepdims=True)
    line[at] = (tokens * lax.rsqrt(squared + EPS) * ffn_gain_ref[...]).astype(BF16)

    def line_copies(which, source, up):
        device = (ep + 2 if up else ep - 2, me)
        way = 0 if up else 1
        pairs = (
            ((marks.at[source], marks.at[source]), (line.at[source], line.at[source]))
            if which == 0
            else (
                (keys.at[2 * source + side], keys.at[2 * source + side]),
                (values.at[2 * source + side], values.at[2 * source + side]),
            )
        )
        return [
            remote(
                pair[0],
                pair[1],
                line_send.at[which, k, way, source],
                line_recv.at[which, k, source],
                device,
            )
            for k, pair in enumerate(pairs)
        ]

    def send_on(which, source):
        @pl.when(at + 1 < half)
        def _():
            for copy in line_copies(which, source, True):
                copy.start()

        @pl.when(at >= 1)
        def _():
            for copy in line_copies(which, source, False):
                copy.start()

    def walk(which, use):
        def step_of(step, carry):
            @pl.when(at - step >= 0)
            def _():
                source = at - step
                for copy in line_copies(which, source, True):
                    copy.wait_recv()

                @pl.when(at + 1 < half)
                def _():
                    for copy in line_copies(which, source, True):
                        copy.start()

                use(source)

            @pl.when(at + step < half)
            def _():
                source = at + step
                for copy in line_copies(which, source, False):
                    copy.wait_recv()

                @pl.when(at >= 1)
                def _():
                    for copy in line_copies(which, source, False):
                        copy.start()

                use(source)

            return carry

        lax.fori_loop(1, half, step_of, 0)

    def walk_drain(which):
        def step_of(step, carry):
            @pl.when((at - step >= 0) & (at + 1 < half))
            def _():
                for copy in line_copies(which, at - step, True):
                    copy.wait_send()

            @pl.when((at + step < half) & (at >= 1))
            def _():
                for copy in line_copies(which, at + step, False):
                    copy.wait_send()

            return carry

        lax.fori_loop(1, half, step_of, 0)

        @pl.when(at + 1 < half)
        def _():
            for copy in line_copies(which, at, True):
                copy.wait_send()

        @pl.when(at >= 1)
        def _():
            for copy in line_copies(which, at, False):
                copy.wait_send()

    def side_rows(source):
        return remote(
            sent.at[source],
            arrived.at[2 * source + side],
            row_send.at[source],
            row_recv.at[source],
            (beside, me),
        )

    slot_at = lax.broadcasted_iota(jnp.int32, (capacity, quarter), 0)

    def select(source):
        mark = marks[source].astype(jnp.int32)
        block = line[source]

        def rows_of(expert):
            place = slot_at + expert * capacity
            spread = jnp.where((place == mark[0:1, :]) | (place == mark[1:2, :]), 1.0, 0.0)
            return jnp.dot(spread.astype(BF16), block, preferred_element_type=F32).astype(BF16)

        sent[source] = rows_of(beside)
        side_rows(source).start()
        arrived[2 * source + side] = rows_of(ep)

    send_on(0, at)
    select(at)

    groups = groups_ref[:, own]
    group_weights = jnp.exp(groups - jnp.max(groups, axis=0, keepdims=True))
    group_prob = group_weights / jnp.sum(group_weights, axis=0, keepdims=True)
    picks = picks_ref[:, own]
    pick_weights = jnp.exp(picks - jnp.max(picks, axis=0, keepdims=True))
    pick_prob = pick_weights / jnp.sum(pick_weights, axis=0, keepdims=True)
    group_at = lax.broadcasted_iota(jnp.int32, groups.shape, 0)
    gates = []
    for k, pick in enumerate((first, second)):
        gate_row = (
            jnp.sum(
                jnp.where(group_at == pick // (n // group_count), group_prob, 0.0),
                axis=0,
                keepdims=True,
            )
            * pick_prob[k : k + 1, :]
        )
        gates.append(
            jnp.sum(jnp.where(row_at == column_at, gate_row, 0.0), axis=1, keepdims=True)
        )

    walk(0, select)

    def side_kv(source):
        place = 2 * source + side
        return [
            remote(keys.at[place], keys.at[place], kv_send.at[0, source], kv_recv.at[0, source], (beside, me)),
            remote(values.at[place], values.at[place], kv_send.at[1, source], kv_recv.at[1, source], (beside, me)),
        ]

    def relay_kv(source):
        for copy in side_kv(source):
            copy.start()

    for copy in locals_:
        copy.wait()
    send_on(1, at)
    relay_kv(at)

    to_across[0].wait_recv()
    relayed[0].start()

    def wait_rows(source, carry):
        side_rows(source).wait_recv()
        return carry

    lax.fori_loop(0, half, wait_rows, 0)
    units = gate_ref.shape[2]

    def hide(place):
        rows = flat_rows(arrived[...])
        gate_part = jnp.dot(rows, w_gate[place], preferred_element_type=F32)
        up_part = jnp.dot(rows, w_up[place], preferred_element_type=F32)
        hidden[place] = (gate_part / (1.0 + jnp.exp(-gate_part)) * up_part).astype(BF16)

    hide(0)
    to_mate[0].wait_recv()
    to_mate[1].wait_recv()
    hide(1)
    to_across[1].wait_recv()
    relayed[1].start()
    hide(2)
    relayed[0].wait_recv()
    relayed[1].wait_recv()
    hide(3)

    walk(1, relay_kv)

    def back_copy(number, step, receive):
        other = lax.rem(ep + step, n)
        expert = other if receive else ep
        return remote(
            results.at[number, other],
            returned.at[number, expert],
            back_send.at[number, step],
            back_recv.at[number, expert],
            (other, me),
        )

    for number in range(CHUNKS):
        to_across[2 + number].wait_recv()
        relayed[2 + number].start()
        to_mate[2 + number].wait_recv()
        total = jnp.zeros((n * capacity, part), F32)
        for place in range(3):
            total += jnp.dot(
                hidden[place], w_down[place, :, columns(number)], preferred_element_type=F32
            )
        relayed[2 + number].wait_recv()
        total += jnp.dot(hidden[3], w_down[3, :, columns(number)], preferred_element_type=F32)
        results[number] = split_rows(total, capacity)

        def start_back(step, carry):
            back_copy(number, step, False).start()
            return carry

        lax.fori_loop(1, n, start_back, 0)
        returned[number, ep] = results[number, ep]

    def wait_kv(source, carry):
        for copy in side_kv(source):
            copy.wait_recv()
        return carry

    lax.fori_loop(0, half, wait_kv, 0)

    blocks = min(n, 8)
    scale = head_qk**-0.5
    share = token_count // tp
    for head in range(local_heads):
        averaged = []
        for way in range(2):
            column = (2 * head + way) * head_qk
            query = query_ref[:, column : column + head_qk]

            def scored(step):
                key_rows = keys[pl.ds(step * blocks, blocks), :, column : column + head_qk]
                return (
                    lax.dot_general(
                        query,
                        key_rows.reshape(blocks * token_count, head_qk),
                        (((1,), (1,)), ((), ())),
                        preferred_element_type=F32,
                    )
                    * scale
                )

            def absorb(step, carry):
                top, mass, sums = carry
                scores = scored(step)
                new_top = jnp.maximum(top, jnp.max(scores, axis=-1, keepdims=True))
                factor = jnp.exp(top - new_top)
                weights = jnp.exp(scores - new_top)
                value_rows = values[
                    pl.ds(step * blocks, blocks), :, head * head_v : (head + 1) * head_v
                ].reshape(blocks * token_count, head_v)
                mass = mass * factor + jnp.sum(weights, axis=-1, keepdims=True)
                sums = sums * factor + jnp.dot(
                    weights.astype(BF16), value_rows, preferred_element_type=F32
                )
                return new_top, mass, sums

            start = (
                jnp.full((token_count, 1), -1e30, F32),
                jnp.zeros((token_count, 1), F32),
                jnp.zeros((token_count, head_v), F32),
            )
            if n == blocks:
                top, mass, sums = absorb(0, start)
            else:
                top, mass, sums = lax.fori_loop(0, n // blocks, absorb, start)
            averaged.append(sums / mass)
        lambda_at = lambda_ref[0, head]
        per_head = averaged[0] - lambda_at * averaged[1]
        squares = jnp.mean(per_head * per_head, axis=-1, keepdims=True)
        normed_head = per_head * lax.rsqrt(squares + EPS) * head_gain_ref[...] * HEAD_SCALE
        attended[:, :, head * head_v : (head + 1) * head_v] = normed_head.astype(BF16).reshape(
            tp, share, head_v
        )

    head_copies = []
    for step in range(1, tp):
        head_copies.append(
            remote(
                attended.at[lax.rem(me + step, tp)],
                collected.at[step],
                head_send.at[step],
                head_recv.at[step],
                (ep, lax.rem(me + step, tp)),
            )
        )
    for copy in head_copies:
        copy.start()
    collected[0] = attended[me]
    depth = local_heads * head_v
    for copy in head_copies:
        copy.wait_recv()
    mixed = jnp.zeros((share, width), F32)
    for step in range(tp):
        from_tp = lax.rem(me - step + tp, tp)
        mixed += jnp.dot(
            collected[step],
            w_out[pl.ds(pl.multiple_of(from_tp * depth, depth), depth), :],
            preferred_element_type=F32,
        )
    mixer_ref[...] = mixed.astype(BF16)

    back_at = lax.broadcasted_iota(jnp.int32, (n * capacity, quarter), 0)
    choose = [
        jnp.where(back_at == slot.astype(jnp.int32), 1.0, 0.0).astype(BF16) for slot in slots
    ]
    over_rows = (((0,), (0,)), ((), ()))
    for number in range(CHUNKS):

        def wait_back(step, carry):
            back_copy(number, step, True).wait_recv()
            return carry

        lax.fori_loop(1, n, wait_back, 0)
        rows = flat_rows(returned[number])
        combined = gates[0] * lax.dot_general(
            choose[0], rows, over_rows, preferred_element_type=F32
        )
        combined += gates[1] * lax.dot_general(
            choose[1], rows, over_rows, preferred_element_type=F32
        )
        out_ref[:, number * part : (number + 1) * part] = combined.astype(BF16)

    for copy in to_across + to_mate + relayed + head_copies:
        copy.wait_send()

    def drain(step, carry):
        for number in range(CHUNKS):
            back_copy(number, step, False).wait_send()
        return carry

    lax.fori_loop(1, n, drain, 0)

    def drain_side(source, carry):
        side_rows(source).wait_send()
        for copy in side_kv(source):
            copy.wait_send()
        return carry

    lax.fori_loop(0, half, drain_side, 0)
    walk_drain(0)
    walk_drain(1)


def local(
    n,
    tp,
    query_rows,
    key_rows,
    value_rows,
    lambdas,
    head_gain,
    w_out,
    moe_rows,
    ffn_gain,
    routes,
    group_logits,
    pick_logits,
    w_gate,
    w_up,
    w_down,
):
    token_count = query_rows.shape[0]
    local_heads = lambdas.shape[1]
    head_qk = query_rows.shape[1] // (2 * local_heads)
    head_v = value_rows.shape[1] // local_heads
    width = moe_rows.shape[1]
    quarter = moe_rows.shape[0] // tp
    capacity = max(2, 2 * routes.shape[0] * quarter // n)
    units = w_gate.shape[2]
    part = width // CHUNKS
    share = token_count // tp
    dims = (token_count, local_heads, head_qk, head_v, quarter, capacity, group_logits.shape[0])
    vmem = pl.BlockSpec(memory_space=pltpu.VMEM)
    anywhere = pl.BlockSpec(memory_space=pl.ANY)
    dma = pltpu.SemaphoreType.DMA
    return pl.pallas_call(
        functools.partial(kernel, n, tp, dims),
        out_shape=(
            jax.ShapeDtypeStruct((share, width), BF16),
            jax.ShapeDtypeStruct((quarter, width), BF16),
        ),
        in_specs=[
            vmem,
            anywhere,
            anywhere,
            pl.BlockSpec(memory_space=pltpu.SMEM),
            vmem,
            anywhere,
            anywhere,
            vmem,
            vmem,
            vmem,
            vmem,
            anywhere,
            anywhere,
            anywhere,
        ],
        out_specs=(vmem, vmem),
        scratch_shapes=[
            pltpu.VMEM((quarter, width), BF16),
            pltpu.VMEM((n // 2, 8, quarter), F32),
            pltpu.VMEM((n // 2, quarter, width), BF16),
            pltpu.VMEM((n // 2, capacity, width), BF16),
            pltpu.VMEM((n, capacity, width), BF16),
            pltpu.VMEM((4, width, units), BF16),
            pltpu.VMEM((4, width, units), BF16),
            pltpu.VMEM((4, units, width), BF16),
            pltpu.VMEM((n, token_count, key_rows.shape[1]), BF16),
            pltpu.VMEM((n, token_count, value_rows.shape[1]), BF16),
            pltpu.VMEM(w_out.shape, BF16),
            pltpu.VMEM((tp, share, local_heads * head_v), BF16),
            pltpu.VMEM((tp, share, local_heads * head_v), BF16),
            pltpu.VMEM((4, n * capacity, units), BF16),
            pltpu.VMEM((CHUNKS, n, capacity, part), BF16),
            pltpu.VMEM((CHUNKS, n, capacity, part), BF16),
            dma((7,)),
            dma((2, 2, 2, n // 2)),
            dma((2, 2, n // 2)),
            dma((3, 2 + CHUNKS)),
            dma((3, 2 + CHUNKS)),
            dma((n // 2,)),
            dma((n // 2,)),
            dma((2, n // 2)),
            dma((2, n // 2)),
            dma((CHUNKS, n)),
            dma((CHUNKS, n)),
            dma((tp,)),
            dma((tp,)),
        ],
        compiler_params=pltpu.CompilerParams(
            collective_id=0, has_side_effects=True, vmem_limit_bytes=60 * 1024 * 1024
        ),
    )(
        query_rows,
        key_rows,
        value_rows,
        lambdas,
        head_gain.reshape(1, -1),
        w_out,
        moe_rows,
        ffn_gain.reshape(1, -1),
        routes,
        group_logits,
        pick_logits,
        w_gate,
        w_up,
        w_down,
    )


def solution(mesh):
    inner = jax.shard_map(
        functools.partial(local, mesh.shape["ep"], mesh.shape["tp"]),
        mesh=mesh,
        in_specs=(
            P("ep", "tp"),
            P("ep", "tp"),
            P("ep", "tp"),
            P(None, "tp"),
            P(),
            P(),
            P("ep", None),
            P(),
            P(None, "ep"),
            P(None, "ep"),
            P(None, "ep"),
            P("ep", None, "tp"),
            P("ep", None, "tp"),
            P("ep", "tp", None),
        ),
        out_specs=(P(("ep", "tp"), None), P(("ep", "tp"), None)),
        check_vma=False,
    )

    def whole(*args):
        args = list(args)
        args[3] = args[3].reshape(1, -1)
        for place in (8, 9, 10):
            args[place] = args[place].T
        return inner(*args)

    return whole
```

```python
import functools

import jax
import jax.numpy as jnp
from jax import lax
from jax.experimental import pallas as pl
from jax.experimental.pallas import tpu as pltpu
from jax.sharding import PartitionSpec as P

EPS = 1e-06
HEAD_SCALE = 0.8
CHUNKS = 8
MESH = pl.DeviceIdType.MESH
F32 = jnp.float32
BF16 = jnp.bfloat16


def flat_rows(values):
    blocks, rows, columns = values.shape
    if rows % 16:
        return values.astype(F32).reshape(blocks * rows, columns).astype(values.dtype)
    return values.reshape(blocks * rows, columns)


def split_rows(values, rows):
    columns = values.shape[1]
    if rows % 16:
        return values.reshape(-1, rows, columns).astype(BF16)
    return values.astype(BF16).reshape(-1, rows, columns)


def kernel(
    n,
    tp,
    dims,
    query_ref,
    key_ref,
    value_ref,
    lambda_ref,
    head_gain_ref,
    w_out_ref,
    moe_ref,
    ffn_gain_ref,
    routes_ref,
    groups_ref,
    picks_ref,
    gate_ref,
    up_ref,
    down_ref,
    mixer_ref,
    out_ref,
    rows_buf,
    marks,
    line,
    sent,
    arrived,
    w_gate,
    w_up,
    w_down,
    keys,
    values,
    w_out,
    attended,
    collected,
    hidden,
    results,
    returned,
    local_sem,
    line_send,
    line_recv,
    weight_send,
    weight_recv,
    row_send,
    row_recv,
    kv_send,
    kv_recv,
    back_send,
    back_recv,
    head_send,
    head_recv,
):
    token_count, local_heads, head_qk, head_v, quarter, capacity, group_count = dims
    ep = lax.axis_index("ep")
    me = lax.axis_index("tp")
    mate = me + 1 - 2 * lax.rem(me, 2)
    across = lax.rem(me + tp // 2, tp)
    diagonal = lax.rem(mate + tp // 2, tp)
    beside = ep + 1 - 2 * lax.rem(ep, 2)
    half = n // 2
    at, side = ep // 2, lax.rem(ep, 2)
    width = out_ref.shape[1]
    part = width // CHUNKS

    def remote(source, target, send, recv, device):
        return pltpu.make_async_remote_copy(
            src_ref=source,
            dst_ref=target,
            send_sem=send,
            recv_sem=recv,
            device_id=device,
            device_id_type=MESH,
        )

    own_rows = pltpu.make_async_copy(
        moe_ref.at[pl.ds(pl.multiple_of(me * quarter, quarter), quarter)], rows_buf, local_sem.at[0]
    )
    own_rows.start()
    locals_ = [
        pltpu.make_async_copy(gate_ref.at[0], w_gate.at[0], local_sem.at[1]),
        pltpu.make_async_copy(up_ref.at[0], w_up.at[0], local_sem.at[2]),
        pltpu.make_async_copy(down_ref.at[0], w_down.at[0], local_sem.at[3]),
        pltpu.make_async_copy(key_ref, keys.at[ep], local_sem.at[4]),
        pltpu.make_async_copy(value_ref, values.at[ep], local_sem.at[5]),
        pltpu.make_async_copy(w_out_ref, w_out, local_sem.at[6]),
    ]
    for copy in locals_:
        copy.start()

    barrier = pltpu.get_barrier_semaphore()
    for peer in (mate, across, diagonal):
        pl.semaphore_signal(barrier, inc=1, device_id=(ep, peer), device_id_type=MESH)

    def greet(step, carry):
        pl.semaphore_signal(
            barrier, inc=1, device_id=(lax.rem(ep + step, n), me), device_id_type=MESH
        )
        return carry

    lax.fori_loop(1, n, greet, 0)
    pl.semaphore_wait(barrier, n - 1 + 3)

    def columns(number):
        return pl.ds(number * part, part)

    def weight_copies(place, first):
        device = (ep, across if place == 2 else mate)
        sources = (
            (gate_ref.at[0], up_ref.at[0], down_ref.at[0])
            if first
            else (w_gate.at[2], w_up.at[2], w_down.at[2])
        )
        base = place - 1
        copies = [
            remote(
                sources[0],
                w_gate.at[place],
                weight_send.at[base, 0],
                weight_recv.at[base, 0],
                device,
            ),
            remote(
                sources[1],
                w_up.at[place],
                weight_send.at[base, 1],
                weight_recv.at[base, 1],
                device,
            ),
        ]
        for number in range(CHUNKS):
            copies.append(
                remote(
                    sources[2].at[:, columns(number)],
                    w_down.at[place, :, columns(number)],
                    weight_send.at[base, 2 + number],
                    weight_recv.at[base, 2 + number],
                    device,
                )
            )
        return copies

    to_across = weight_copies(2, True)
    to_mate = weight_copies(1, True)
    relayed = weight_copies(3, False)
    for copy in to_across:
        copy.start()
    for copy in to_mate:
        copy.start()

    own = pl.ds(pl.multiple_of(me * quarter, quarter), quarter)
    routes = routes_ref[:, own]
    first, second = routes[0:1, :], routes[1:2, :]
    experts = lax.broadcasted_iota(jnp.int32, (n, quarter), 0)
    named = jnp.where((experts == first) | (experts == second), 1.0, 0.0)
    row_at = lax.broadcasted_iota(jnp.int32, (quarter, quarter), 0)
    column_at = lax.broadcasted_iota(jnp.int32, (quarter, quarter), 1)
    earlier = jnp.where(row_at < column_at, 1.0, 0.0).astype(BF16)
    before = jnp.dot(named.astype(BF16), earlier, preferred_element_type=F32)
    slots = [
        (pick * capacity).astype(F32)
        + jnp.sum(jnp.where(experts == pick, before, 0.0), axis=0, keepdims=True)
        for pick in (first, second)
    ]
    mark_at = lax.broadcasted_iota(jnp.int32, (8, quarter), 0)
    marks[at] = jnp.where(mark_at == 0, slots[0], slots[1])

    own_rows.wait()
    tokens = rows_buf[...].astype(F32)
    squared = jnp.mean(tokens * tokens, axis=-1, keepdims=True)
    line[at] = (tokens * lax.rsqrt(squared + EPS) * ffn_gain_ref[...]).astype(BF16)

    def line_copies(which, source, up):
        device = (ep + 2 if up else ep - 2, me)
        way = 0 if up else 1
        pairs = (
            ((marks.at[source], marks.at[source]), (line.at[source], line.at[source]))
            if which == 0
            else (
                (keys.at[2 * source + side], keys.at[2 * source + side]),
                (values.at[2 * source + side], values.at[2 * source + side]),
            )
        )
        return [
            remote(
                pair[0],
                pair[1],
                line_send.at[which, k, way, source],
                line_recv.at[which, k, source],
                device,
            )
            for k, pair in enumerate(pairs)
        ]

    def send_on(which, source):
        @pl.when(at + 1 < half)
        def _():
            for copy in line_copies(which, source, True):
                copy.start()

        @pl.when(at >= 1)
        def _():
            for copy in line_copies(which, source, False):
                copy.start()

    def walk(which, use):
        def step_of(step, carry):
            @pl.when(at - step >= 0)
            def _():
                source = at - step
                for copy in line_copies(which, source, True):
                    copy.wait_recv()

                @pl.when(at + 1 < half)
                def _():
                    for copy in line_copies(which, source, True):
                        copy.start()

                use(source)

            @pl.when(at + step < half)
            def _():
                source = at + step
                for copy in line_copies(which, source, False):
                    copy.wait_recv()

                @pl.when(at >= 1)
                def _():
                    for copy in line_copies(which, source, False):
                        copy.start()

                use(source)

            return carry

        lax.fori_loop(1, half, step_of, 0)

    def walk_drain(which):
        def step_of(step, carry):
            @pl.when((at - step >= 0) & (at + 1 < half))
            def _():
                for copy in line_copies(which, at - step, True):
                    copy.wait_send()

            @pl.when((at + step < half) & (at >= 1))
            def _():
                for copy in line_copies(which, at + step, False):
                    copy.wait_send()

            return carry

        lax.fori_loop(1, half, step_of, 0)

        @pl.when(at + 1 < half)
        def _():
            for copy in line_copies(which, at, True):
                copy.wait_send()

        @pl.when(at >= 1)
        def _():
            for copy in line_copies(which, at, False):
                copy.wait_send()

    def side_rows(source):
        return remote(
            sent.at[source],
            arrived.at[2 * source + side],
            row_send.at[source],
            row_recv.at[source],
            (beside, me),
        )

    slot_at = lax.broadcasted_iota(jnp.int32, (capacity, quarter), 0)

    def select(source):
        mark = marks[source].astype(jnp.int32)
        block = line[source]

        def rows_of(expert):
            place = slot_at + expert * capacity
            spread = jnp.where((place == mark[0:1, :]) | (place == mark[1:2, :]), 1.0, 0.0)
            return jnp.dot(spread.astype(BF16), block, preferred_element_type=F32).astype(BF16)

        sent[source] = rows_of(beside)
        side_rows(source).start()
        arrived[2 * source + side] = rows_of(ep)

    send_on(0, at)
    select(at)

    groups = groups_ref[:, own]
    group_weights = jnp.exp(groups - jnp.max(groups, axis=0, keepdims=True))
    group_prob = group_weights / jnp.sum(group_weights, axis=0, keepdims=True)
    picks = picks_ref[:, own]
    pick_weights = jnp.exp(picks - jnp.max(picks, axis=0, keepdims=True))
    pick_prob = pick_weights / jnp.sum(pick_weights, axis=0, keepdims=True)
    group_at = lax.broadcasted_iota(jnp.int32, groups.shape, 0)
    gates = []
    for k, pick in enumerate((first, second)):
        gate_row = (
            jnp.sum(
                jnp.where(group_at == pick // (n // group_count), group_prob, 0.0),
                axis=0,
                keepdims=True,
            )
            * pick_prob[k : k + 1, :]
        )
        gates.append(
            jnp.sum(jnp.where(row_at == column_at, gate_row, 0.0), axis=1, keepdims=True)
        )

    walk(0, select)

    def side_kv(source):
        place = 2 * source + side
        return [
            remote(keys.at[place], keys.at[place], kv_send.at[0, source], kv_recv.at[0, source], (beside, me)),
            remote(values.at[place], values.at[place], kv_send.at[1, source], kv_recv.at[1, source], (beside, me)),
        ]

    def relay_kv(source):
        for copy in side_kv(source):
            copy.start()

    for copy in locals_:
        copy.wait()
    send_on(1, at)
    relay_kv(at)

    to_across[0].wait_recv()
    relayed[0].start()

    def wait_rows(source, carry):
        side_rows(source).wait_recv()
        return carry

    lax.fori_loop(0, half, wait_rows, 0)
    units = gate_ref.shape[2]

    def hide(place):
        rows = flat_rows(arrived[...])
        gate_part = jnp.dot(rows, w_gate[place], preferred_element_type=F32)
        up_part = jnp.dot(rows, w_up[place], preferred_element_type=F32)
        hidden[place] = (gate_part / (1.0 + jnp.exp(-gate_part)) * up_part).astype(BF16)

    hide(0)
    to_mate[0].wait_recv()
    to_mate[1].wait_recv()
    hide(1)
    to_across[1].wait_recv()
    relayed[1].start()
    hide(2)
    relayed[0].wait_recv()
    relayed[1].wait_recv()
    hide(3)

    walk(1, relay_kv)

    def back_copy(number, step, receive):
        other = lax.rem(ep + step, n)
        expert = other if receive else ep
        return remote(
            results.at[number, other],
            returned.at[number, expert],
            back_send.at[number, step],
            back_recv.at[number, expert],
            (other, me),
        )

    for number in range(CHUNKS):
        to_across[2 + number].wait_recv()
        relayed[2 + number].start()
        to_mate[2 + number].wait_recv()
        total = jnp.zeros((n * capacity, part), F32)
        for place in range(3):
            total += jnp.dot(
                hidden[place], w_down[place, :, columns(number)], preferred_element_type=F32
            )
        relayed[2 + number].wait_recv()
        total += jnp.dot(hidden[3], w_down[3, :, columns(number)], preferred_element_type=F32)
        results[number] = split_rows(total, capacity)

        def start_back(step, carry):
            back_copy(number, step, False).start()
            return carry

        lax.fori_loop(1, n, start_back, 0)
        returned[number, ep] = results[number, ep]

    def wait_kv(source, carry):
        for copy in side_kv(source):
            copy.wait_recv()
        return carry

    lax.fori_loop(0, half, wait_kv, 0)

    blocks = min(n, 8)
    scale = head_qk**-0.5
    share = token_count // tp
    for head in range(local_heads):
        averaged = []
        for way in range(2):
            column = (2 * head + way) * head_qk
            query = query_ref[:, column : column + head_qk]

            def scored(step):
                key_rows = keys[pl.ds(step * blocks, blocks), :, column : column + head_qk]
                return (
                    lax.dot_general(
                        query,
                        key_rows.reshape(blocks * token_count, head_qk),
                        (((1,), (1,)), ((), ())),
                        preferred_element_type=F32,
                    )
                    * scale
                )

            def absorb(step, carry):
                top, mass, sums = carry
                scores = scored(step)
                new_top = jnp.maximum(top, jnp.max(scores, axis=-1, keepdims=True))
                factor = jnp.exp(top - new_top)
                weights = jnp.exp(scores - new_top)
                value_rows = values[
                    pl.ds(step * blocks, blocks), :, head * head_v : (head + 1) * head_v
                ].reshape(blocks * token_count, head_v)
                mass = mass * factor + jnp.sum(weights, axis=-1, keepdims=True)
                sums = sums * factor + jnp.dot(
                    weights.astype(BF16), value_rows, preferred_element_type=F32
                )
                return new_top, mass, sums

            start = (
                jnp.full((token_count, 1), -1e30, F32),
                jnp.zeros((token_count, 1), F32),
                jnp.zeros((token_count, head_v), F32),
            )
            if n == blocks:
                top, mass, sums = absorb(0, start)
            else:
                top, mass, sums = lax.fori_loop(0, n // blocks, absorb, start)
            averaged.append(sums / mass)
        lambda_at = lambda_ref[0, head]
        per_head = averaged[0] - lambda_at * averaged[1]
        squares = jnp.mean(per_head * per_head, axis=-1, keepdims=True)
        normed_head = per_head * lax.rsqrt(squares + EPS) * head_gain_ref[...] * HEAD_SCALE
        attended[:, :, head * head_v : (head + 1) * head_v] = normed_head.astype(BF16).reshape(
            tp, share, head_v
        )

    head_copies = []
    for step in range(1, tp):
        head_copies.append(
            remote(
                attended.at[lax.rem(me + step, tp)],
                collected.at[step],
                head_send.at[step],
                head_recv.at[step],
                (ep, lax.rem(me + step, tp)),
            )
        )
    for copy in head_copies:
        copy.start()
    collected[0] = attended[me]
    depth = local_heads * head_v
    for copy in head_copies:
        copy.wait_recv()
    mixed = jnp.zeros((share, width), F32)
    for step in range(tp):
        from_tp = lax.rem(me - step + tp, tp)
        mixed += jnp.dot(
            collected[step],
            w_out[pl.ds(pl.multiple_of(from_tp * depth, depth), depth), :],
            preferred_element_type=F32,
        )
    mixer_ref[...] = mixed.astype(BF16)

    back_at = lax.broadcasted_iota(jnp.int32, (n * capacity, quarter), 0)
    choose = [
        jnp.where(back_at == slot.astype(jnp.int32), 1.0, 0.0).astype(BF16) for slot in slots
    ]
    over_rows = (((0,), (0,)), ((), ()))
    for number in range(CHUNKS):

        def wait_back(step, carry):
            back_copy(number, step, True).wait_recv()
            return carry

        lax.fori_loop(1, n, wait_back, 0)
        rows = flat_rows(returned[number])
        combined = gates[0] * lax.dot_general(
            choose[0], rows, over_rows, preferred_element_type=F32
        )
        combined += gates[1] * lax.dot_general(
            choose[1], rows, over_rows, preferred_element_type=F32
        )
        out_ref[:, number * part : (number + 1) * part] = combined.astype(BF16)

    for copy in to_across + to_mate + relayed + head_copies:
        copy.wait_send()

    def drain(step, carry):
        for number in range(CHUNKS):
            back_copy(number, step, False).wait_send()
        return carry

    lax.fori_loop(1, n, drain, 0)

    def drain_side(source, carry):
        side_rows(source).wait_send()
        for copy in side_kv(source):
            copy.wait_send()
        return carry

    lax.fori_loop(0, half, drain_side, 0)
    walk_drain(0)
    walk_drain(1)


def hand_over(mixed_ref, combined_ref, mixer_ref, out_ref):
    mixer_ref[...] = mixed_ref[...]
    out_ref[...] = combined_ref[...]


def local(
    n,
    tp,
    query_rows,
    key_rows,
    value_rows,
    lambdas,
    head_gain,
    w_out,
    moe_rows,
    ffn_gain,
    routes,
    group_logits,
    pick_logits,
    w_gate,
    w_up,
    w_down,
):
    token_count = query_rows.shape[0]
    local_heads = lambdas.shape[1]
    head_qk = query_rows.shape[1] // (2 * local_heads)
    head_v = value_rows.shape[1] // local_heads
    width = moe_rows.shape[1]
    quarter = moe_rows.shape[0] // tp
    capacity = max(2, 2 * routes.shape[0] * quarter // n)
    units = w_gate.shape[2]
    part = width // CHUNKS
    share = token_count // tp
    dims = (token_count, local_heads, head_qk, head_v, quarter, capacity, group_logits.shape[0])
    vmem = pl.BlockSpec(memory_space=pltpu.VMEM)
    anywhere = pl.BlockSpec(memory_space=pl.ANY)
    dma = pltpu.SemaphoreType.DMA
    mixed, combined = pl.pallas_call(
        functools.partial(kernel, n, tp, dims),
        out_shape=(
            jax.ShapeDtypeStruct((share, width), BF16),
            jax.ShapeDtypeStruct((quarter, width), BF16),
        ),
        in_specs=[
            vmem,
            anywhere,
            anywhere,
            pl.BlockSpec(memory_space=pltpu.SMEM),
            vmem,
            anywhere,
            anywhere,
            vmem,
            vmem,
            vmem,
            vmem,
            anywhere,
            anywhere,
            anywhere,
        ],
        out_specs=(vmem, vmem),
        scratch_shapes=[
            pltpu.VMEM((quarter, width), BF16),
            pltpu.VMEM((n // 2, 8, quarter), F32),
            pltpu.VMEM((n // 2, quarter, width), BF16),
            pltpu.VMEM((n // 2, capacity, width), BF16),
            pltpu.VMEM((n, capacity, width), BF16),
            pltpu.VMEM((4, width, units), BF16),
            pltpu.VMEM((4, width, units), BF16),
            pltpu.VMEM((4, units, width), BF16),
            pltpu.VMEM((n, token_count, key_rows.shape[1]), BF16),
            pltpu.VMEM((n, token_count, value_rows.shape[1]), BF16),
            pltpu.VMEM(w_out.shape, BF16),
            pltpu.VMEM((tp, share, local_heads * head_v), BF16),
            pltpu.VMEM((tp, share, local_heads * head_v), BF16),
            pltpu.VMEM((4, n * capacity, units), BF16),
            pltpu.VMEM((CHUNKS, n, capacity, part), BF16),
            pltpu.VMEM((CHUNKS, n, capacity, part), BF16),
            dma((7,)),
            dma((2, 2, 2, n // 2)),
            dma((2, 2, n // 2)),
            dma((3, 2 + CHUNKS)),
            dma((3, 2 + CHUNKS)),
            dma((n // 2,)),
            dma((n // 2,)),
            dma((2, n // 2)),
            dma((2, n // 2)),
            dma((CHUNKS, n)),
            dma((CHUNKS, n)),
            dma((tp,)),
            dma((tp,)),
        ],
        compiler_params=pltpu.CompilerParams(
            collective_id=0, has_side_effects=True, vmem_limit_bytes=60 * 1024 * 1024
        ),
    )(
        query_rows,
        key_rows,
        value_rows,
        lambdas,
        head_gain.reshape(1, -1),
        w_out,
        moe_rows,
        ffn_gain.reshape(1, -1),
        routes,
        group_logits,
        pick_logits,
        w_gate,
        w_up,
        w_down,
    )
    return pl.pallas_call(
        hand_over,
        out_shape=(
            jax.ShapeDtypeStruct(mixed.shape, BF16),
            jax.ShapeDtypeStruct(combined.shape, BF16),
        ),
        in_specs=[vmem, vmem],
        out_specs=(vmem, vmem),
        compiler_params=pltpu.CompilerParams(vmem_limit_bytes=8 * 1024 * 1024),
    )(mixed, combined)


def solution(mesh):
    inner = jax.shard_map(
        functools.partial(local, mesh.shape["ep"], mesh.shape["tp"]),
        mesh=mesh,
        in_specs=(
            P("ep", "tp"),
            P("ep", "tp"),
            P("ep", "tp"),
            P(None, "tp"),
            P(),
            P(),
            P("ep", None),
            P(),
            P(None, "ep"),
            P(None, "ep"),
            P(None, "ep"),
            P("ep", None, "tp"),
            P("ep", None, "tp"),
            P("ep", "tp", None),
        ),
        out_specs=(P(("ep", "tp"), None), P(("ep", "tp"), None)),
        check_vma=False,
    )

    def whole(*args):
        args = list(args)
        args[3] = args[3].reshape(1, -1)
        for place in (8, 9, 10):
            args[place] = args[place].T
        return inner(*args)

    return whole
```
